128 devices in a mesh: ep: 16 (over z, x), tp: 8 (over y, core).
Axes of the slice: x: 4, y: 4, z: 4, core: 2. Of those that a mesh axis runs over, the one named last changes fastest.
Arguments:
- tokens: bfloat16 [16384, 2048], P(('ep', 'tp')), may hold values from -6 to 6
- expert_ids: int32 [16384, 4], P('ep'), may hold values from 0 to 15, all different within a row; in each aligned block of 128 rows (0 to 127, 128 to 255, ...) at most 64 rows name the same one
- gate_values: float32 [16384, 4], P('ep'), may hold values from 0.1 to 1
- norm_gain: float32 [2048], replicated, may hold values from 0.1 to 1.9
- gate_weight: bfloat16 [16, 2048, 1024], P('ep', None, 'tp'), may hold values from -0.125 to 0.125
- up_weight: bfloat16 [16, 2048, 1024], P('ep', None, 'tp'), may hold values from -0.125 to 0.125
- down_weight: bfloat16 [16, 1024, 2048], P('ep', 'tp'), may hold values from -0.1875 to 0.1875
- out_gain: float32 [2048], P('tp'), may hold values from 0.1 to 1.9
Outputs:
- mixed: bfloat16 [16384, 2048], P('ep', 'tp')
The draws below stay inside these ranges and needn't reach their ends.
Inputs may be any that keep to these rules, and one draw needn't show every extreme that they name: `expert_ids`: each row names 4 different experts of 0 to 15; within the rows of one device (aligned blocks of 128 rows) no expert is named more than 64 times, and in some blocks one expert is named exactly 64 times.
All inputs are finite; a program needn't handle non-finite values.
Results may differ from the reference program's by a relative error of at most 0.0025.
Values may be sent and summed in bfloat16 or wider, within the bound.
A program may use at most 64 MiB of HBM per device.

```python
import math
import jax
import jax.numpy as jnp
import numpy as np
from jax import lax

D = 2048
FF = 1024
TOP = 4
TOK_DEV = 128
CAP = 64
EXPERTS = 16
TOKENS = 16384
N_EP = 16
N_TP = 8


def level_of(rng, extent, split, least, largest):
    factor_of = 1.0
    for dim, parts in split:
        heights = jax.random.uniform(jax.random.fold_in(jax.random.fold_in(rng, 6), dim), (parts,), jnp.float32, least / len(split), largest / len(split))
        factor_of = factor_of * jnp.repeat(jnp.exp(heights), extent[dim] // parts).reshape((-1,) + (1,) * (len(extent) - 1 - dim))
    return factor_of


def routed_block(own_key, own, number, rows, count, top, limit, lean):
    order = jax.random.permutation(own_key, count)
    heavy_load, usual = load_shares(count, rows * top, limit, lean, True), load_shares(count, rows * top, limit, lean, False)
    places = jnp.arange(count)

    def named(tallies, rotation):
        used = int((tallies > 0).sum())
        fixed = max(1, used // 4)
        shifted = fixed + (places - fixed + rotation * (used - fixed)) % max(1, count - fixed)
        return jnp.zeros((count,), jnp.int32).at[order[jnp.where(places < fixed, places, shifted)]].set(jnp.asarray(tallies, jnp.int32))

    tallies = jnp.where(number % 4 == 0, named(heavy_load, number // 4), named(usual, number - number // 4 - 1))
    mixed = jax.random.permutation(jax.random.fold_in(own, 3), count)
    source_of, sink = mixed[0:count // 2 * 2:2], mixed[1:count // 2 * 2:2]
    slack = jnp.minimum(tallies[source_of] - 1, limit - tallies[sink]) // 2
    slack = jnp.where((source_of == order[0]) | (sink == order[0]) | (tallies[sink] == 0), 0, jnp.maximum(slack, 0))
    shifted = jax.random.randint(jax.random.fold_in(own, 4), (count // 2,), 0, 1 << 20) % (slack + 1)
    tallies = tallies.at[source_of].add(-shifted).at[sink].add(shifted)
    items = jnp.searchsorted(jnp.cumsum(tallies), jnp.arange(rows * top), side="right").astype(jnp.int32)
    table = items.reshape(top, rows).T
    table = table[jax.random.permutation(jax.random.fold_in(own, 1), rows)]
    rotation = jax.random.randint(jax.random.fold_in(own, 2), (rows, 1), 0, top)
    return jnp.take_along_axis(table, (jnp.arange(top)[None, :] + rotation) % top, axis=1)


def load_shares(number_of, total, limit, lean, full):
    portions = [(1 << 20) // math.isqrt(standing ** lean) + 1 for standing in range(1, number_of + 1)]
    largest = limit if full else min(limit, max(-(-total // number_of), total * portions[0] // sum(portions)))
    least = 1 if total - largest >= number_of - 1 else 0
    given, surplus = [largest] + [least] * (number_of - 1), total - largest - least * (number_of - 1)
    while surplus > 0:
        candidates = [i for i in range(1, number_of) if given[i] < largest] or [i for i in range(1, number_of) if given[i] < limit]
        mass, left = sum([portions[i] for i in candidates]), surplus
        for i in candidates:
            addition = min(limit - given[i], max(1, left * portions[i] // mass), surplus)
            given[i] = given[i] + addition
            surplus = surplus - addition
    return np.array(given)


def centred(key, dims, width, bound, pieces=(), held_as=jnp.bfloat16):
    values = width * jax.random.normal(key, dims, jnp.float32)
    if pieces:
        values = values * level_of(key, dims, pieces, -0.22, 0.18)
    return jnp.clip(values, -bound, bound).astype(held_as)


def setup_inputs(seed: int = 0) -> dict:
    key_of = jax.random.split(jax.random.key(seed), 9)
    tokens = centred(key_of[0], (TOKENS, D), 1.0, 6.0, ((0, 128),))
    expert_ids_keys = jax.random.split(jax.random.fold_in(key_of[1], 1), TOKENS // TOK_DEV)
    expert_ids_turns = jax.random.permutation(jax.random.fold_in(key_of[1], 3), TOKENS // TOK_DEV)
    expert_ids = jax.vmap(lambda own, number: routed_block(jax.random.fold_in(key_of[1], 2), own, number, TOK_DEV, EXPERTS, TOP, CAP, 2))(expert_ids_keys, expert_ids_turns).reshape((TOKENS, TOP))
    gate_values = jnp.clip(0.1 + 0.9 * jax.random.uniform(key_of[2], (TOKENS, TOP), jnp.float32) ** level_of(key_of[2], (TOKENS, TOP), ((0, 16),), -0.2, 0.2), 0.1, 1.0)
    norm_gain = jnp.clip(1.0 + 0.18 * jax.random.normal(key_of[3], (D,), jnp.float32), 0.1, 1.9)
    gate_weight = centred(key_of[4], (EXPERTS, D, FF), D ** -0.5, 0.125, ((0, 16), (2, 8)))
    up_weight = centred(key_of[5], (EXPERTS, D, FF), D ** -0.5, 0.125, ((0, 16), (2, 8)))
    down_weight = centred(key_of[6], (EXPERTS, FF, D), FF ** -0.5, 0.1875, ((0, 16), (1, 8)))
    out_gain = jnp.clip(1.0 + 0.18 * jax.random.normal(key_of[7], (D,), jnp.float32), 0.1, 1.9)
    return dict(tokens=tokens, expert_ids=expert_ids, gate_values=gate_values, norm_gain=norm_gain, gate_weight=gate_weight, up_weight=up_weight, down_weight=down_weight, out_gain=out_gain)


epsilon = 1e-05
clamp_limit = 7.0
sigmoid_alpha = 1.702

def rms_rows(values, gain):
    mean_sq = lax.optimization_barrier(jnp.mean(values * values, axis=-1, keepdims=True))
    return values * lax.rsqrt(mean_sq + epsilon) * gain

def clamped_unit(gate_part, up_part):
    glu_part = jnp.minimum(gate_part, clamp_limit)
    lin_part = jnp.clip(up_part, -clamp_limit, clamp_limit)
    return glu_part * jax.nn.sigmoid(sigmoid_alpha * glu_part) * (lin_part + 1.0)

def reference(tokens, expert_ids, gate_values, norm_gain, gate_weight, up_weight, down_weight, out_gain):
    normed = rms_rows(tokens.astype(jnp.float32), norm_gain).astype(jnp.bfloat16)
    blocks = expert_ids.reshape(N_EP * N_TP, TOK_DEV * TOP)
    onehot = (blocks[:, :, None] == jnp.arange(EXPERTS, dtype=jnp.int32)[None, None, :]).astype(jnp.int32)
    slot_num = lax.optimization_barrier(jnp.sum((jnp.cumsum(onehot, axis=1) - onehot) * onehot, axis=2)).reshape(TOKENS, TOP)
    source = (jnp.arange(TOKENS, dtype=jnp.int32) // TOK_DEV)[:, None]
    position = (source * CAP + slot_num).astype(jnp.int32)
    table_rows = N_EP * N_TP * CAP
    token_index = jnp.broadcast_to(jnp.arange(TOKENS, dtype=jnp.int32)[:, None], (TOKENS, TOP)).reshape(-1)
    padded = jnp.concatenate([normed, jnp.zeros((1, D), jnp.bfloat16)], axis=0)

    def one_expert(running, inputs):
        expert, w_gate, w_up, w_down = inputs
        chosen = expert_ids == expert
        where_row = jnp.where(chosen, position, table_rows).astype(jnp.int32)
        owner_row = jnp.full((table_rows + 1,), TOKENS, jnp.int32).at[where_row.reshape(-1)].set(token_index)
        rows_in = padded[owner_row[:table_rows]].astype(jnp.float32)
        gate_part = jnp.dot(rows_in, w_gate.astype(jnp.float32), precision=lax.Precision.HIGHEST)
        up_part = jnp.dot(rows_in, w_up.astype(jnp.float32), precision=lax.Precision.HIGHEST)
        activated = clamped_unit(gate_part, up_part).astype(jnp.bfloat16)
        activated = lax.optimization_barrier(activated).astype(jnp.float32)
        outputs = jnp.dot(activated, w_down.astype(jnp.float32), precision=lax.Precision.HIGHEST).astype(jnp.bfloat16)
        outputs = lax.optimization_barrier(outputs).astype(jnp.float32)
        outputs = jnp.concatenate([outputs, jnp.zeros((1, D), jnp.float32)], axis=0)
        for choice_k in range(TOP):
            weight = jnp.where(chosen[:, choice_k], gate_values[:, choice_k], jnp.float32(0.0))
            running = running + weight[:, None] * outputs[where_row[:, choice_k]]
        return (running, None)
    combined, _ = lax.scan(one_expert, jnp.zeros((TOKENS, D), jnp.float32), (jnp.arange(EXPERTS, dtype=jnp.int32), gate_weight, up_weight, down_weight))
    mean_sq = lax.optimization_barrier(jnp.mean(combined * combined, axis=1, keepdims=True))
    return (combined * lax.rsqrt(mean_sq + epsilon) * out_gain).astype(jnp.bfloat16)
```

```python
import jax
import jax.numpy as jnp
from jax import lax
from jax.experimental import pallas as pl
from jax.experimental.pallas import tpu as pltpu
from jax.sharding import PartitionSpec as P

MESH = pl.DeviceIdType.MESH
F32, BF16 = jnp.float32, jnp.bfloat16
EPS = 1e-05
LIMIT = 7.0
ALPHA = 1.702
SIDE = 4
NEP, NTP = 16, 8
GROUP_ORDER = (0, 1, 3, 2)


def dot(a, b):
    return jnp.dot(a, b, preferred_element_type=F32)


def kernel(
    tok_hbm, ids_ref, gates_ref, ngain_ref, wg_hbm, wu_hbm, wd_hbm, ogain_ref, out_hbm,
    tok, normed, pbuf, vref, gref, snd, xbuf, wg, wu, wd, act, res, ret, wmat, comb, mix, ogbuf,
    loc_sem, wl_s, wr_s, wy_s, wc_s, wi_r, wc_r, disp_s, disp_r, back_s, back_r, fin_s, fin_r, og_s, og_r,
):
    toks, width = tok.shape
    cap = toks // 2
    rows_g = SIDE * cap
    unit = wg.shape[2]
    slice_w = mix.shape[2]
    tiles = width // 256

    ep = lax.axis_index("ep")
    tp = lax.axis_index("tp")
    z, x = ep // SIDE, ep % SIDE
    y, core = tp // 2, tp % 2

    def peer(dz, dx):
        return ((z + dz) % SIDE) * SIDE + (x + dx) % SIDE

    right = ((y + 1) % SIDE) * 2 + core
    left = ((y + SIDE - 1) % SIDE) * 2 + core
    partner = y * 2 + 1 - core

    barrier = pltpu.get_barrier_semaphore()

    @pl.loop(1, NEP)
    def _(r):
        pl.semaphore_signal(
            barrier, inc=1, device_id=(peer(r // SIDE, r % SIDE), tp), device_id_type=MESH
        )

    @pl.loop(1, NTP)
    def _(k):
        pl.semaphore_signal(barrier, inc=1, device_id=(ep, (tp + k) % NTP), device_id_type=MESH)

    load_tok = pltpu.make_async_copy(tok_hbm, tok, loc_sem.at[0])
    load_tok.start()
    bufs = (wg, wu, wd)
    srcs = (wg_hbm.at[0], wu_hbm.at[0], wd_hbm.at[0])
    load_w = [
        pltpu.make_async_copy(srcs[p], bufs[p].at[core], loc_sem.at[1 + p]) for p in range(3)
    ]
    for cp in load_w:
        cp.start()
    pl.semaphore_wait(barrier, NEP - 1 + NTP - 1)

    def remote(src, dst, send, recv, ep_to, tp_to):
        return pltpu.make_async_remote_copy(
            src_ref=src, dst_ref=dst, send_sem=send, recv_sem=recv,
            device_id=(ep_to, tp_to), device_id_type=MESH,
        )

    def own_right(p):
        return remote(srcs[p], bufs[p].at[2 + core], wr_s.at[p], wi_r.at[p, 0], ep, right)

    def own_left(p):
        return remote(srcs[p], bufs[p].at[4 + core], wl_s.at[p], wi_r.at[p, 1], ep, left)

    def relay(p):
        return remote(
            bufs[p].at[2 + 2 * core + core], bufs[p].at[6 + core], wy_s.at[p], wi_r.at[p, 2],
            ep, right + core * (left - right),
        )

    def cross(p, j):
        src = srcs[p] if j == 0 else bufs[p].at[2 * j + core]
        return remote(src, bufs[p].at[2 * j + core], wc_s.at[p, j], wc_r.at[p, j], ep, partner)

    def from_partner(p, j):
        slot = bufs[p].at[2 * j + 1 - core]
        return remote(slot, slot, wc_s.at[p, j], wc_r.at[p, j], ep, partner)

    for p in range(2):
        own_right(p).start()
        own_left(p).start()
    for p in range(2):
        cross(p, 0).start()

    ogbuf[tp] = ogain_ref[...]

    def og_copy(k, frm, to):
        return remote(ogain_ref, ogbuf.at[frm], og_s.at[k], og_r.at[k], ep, to)

    @pl.loop(1, NTP)
    def _(k):
        og_copy(k, tp, (tp + k) % NTP).start()

    own = pl.ds(pl.multiple_of(tp * toks, toks), toks)
    ids = ids_ref[:, own]
    gates = gates_ref[:, own]
    rel = lax.broadcasted_iota(jnp.int32, (NEP, toks), 0)
    expert = ((z + rel // SIDE) % SIDE) * SIDE + (x + rel % SIDE) % SIDE
    named = jnp.zeros((NEP, toks), F32)
    gate_of = jnp.zeros((NEP, toks), F32)
    for k in range(ids.shape[0]):
        hit = ids[k : k + 1, :] == expert
        named = jnp.where(hit, 1.0, named)
        gate_of = jnp.where(hit, gates[k : k + 1, :], gate_of)
    t_from = lax.broadcasted_iota(jnp.int32, (toks, toks), 0)
    t_to = lax.broadcasted_iota(jnp.int32, (toks, toks), 1)
    earlier = jnp.where(t_from < t_to, 1.0, 0.0).astype(BF16)
    slot = dot(named.astype(BF16), earlier)
    vref[...] = jnp.where(named > 0.0, slot, -1.0)
    gref[...] = gate_of
    slot_iota = lax.broadcasted_iota(jnp.int32, (cap, toks), 0).astype(F32)

    @pl.loop(0, NEP)
    def _(r):
        pick = jnp.where(vref[pl.ds(r, 1), :] == slot_iota, 1.0, 0.0)
        pbuf[pl.ds(pl.multiple_of(r * cap, cap), cap), :] = pick.astype(BF16)

    load_tok.wait()
    ngain = ngain_ref[...]

    @pl.loop(0, toks // 16)
    def _(i):
        strip = pl.ds(pl.multiple_of(i * 16, 16), 16)
        v = tok[strip, :].astype(F32)
        ms = jnp.mean(v * v, axis=-1, keepdims=True)
        normed[strip, :] = (v * lax.rsqrt(ms + EPS) * ngain).astype(BF16)

    def dispatch(r):
        part = pl.ds(pl.multiple_of(r * cap, cap), cap)
        return remote(
            snd.at[part, :], xbuf.at[part, :], disp_s.at[r], disp_r.at[r],
            peer(r // SIDE, r % SIDE), tp,
        )

    for g in (2, 1, 3, 0):
        group = pl.ds(g * rows_g, rows_g)

        @pl.loop(0, tiles)
        def _(n):
            cols = pl.ds(pl.multiple_of(n * 256, 256), 256)
            picked = dot(pbuf[group, :], normed[:, cols]).astype(BF16)
            if g == 0:
                xbuf[0:cap, cols] = picked[0:cap, :]
                snd[cap:rows_g, cols] = picked[cap:rows_g, :]
            else:
                snd[group, cols] = picked

        for dx in (2, 1, 3, 0):
            if g or dx:
                dispatch(g * SIDE + dx).start()

    @pl.loop(0, NEP // 2)
    def _(q):
        halves = [
            jnp.where(
                vref[pl.ds(2 * q + h, 1), :] == slot_iota, gref[pl.ds(2 * q + h, 1), :], 0.0
            )
            for h in range(2)
        ]
        w = jnp.concatenate(halves, axis=0).T
        cols = pl.ds(pl.multiple_of(q * 2 * cap, 2 * cap), 2 * cap)
        for s in range(3):
            term = w.astype(BF16)
            wmat[s * toks : (s + 1) * toks, cols] = term
            w = w - term.astype(F32)

    def gate_up(g, j):
        rows = pl.ds(pl.multiple_of(g * rows_g, rows_g), rows_g)
        xg = xbuf[rows, :]
        gate_part = dot(xg, jnp.concatenate([wg[2 * j], wg[2 * j + 1]], axis=1))
        up_part = dot(xg, jnp.concatenate([wu[2 * j], wu[2 * j + 1]], axis=1))
        gl = jnp.minimum(gate_part, LIMIT)
        li = jnp.clip(up_part, -LIMIT, LIMIT)
        fresh = gl * jax.nn.sigmoid(ALPHA * gl) * (li + 1.0)
        act[rows, pl.ds(pl.multiple_of(j * 2 * unit, 2 * unit), 2 * unit)] = fresh.astype(BF16)

    def rows_here(g):
        for dx in range(SIDE):
            if g or dx:
                dispatch(g * SIDE + dx).wait_recv()

    def pass_on(p, first):
        own_right(p).wait_recv()
        own_left(p).wait_recv()
        relay(p).start()
        cross(p, 1).start()
        cross(p, 2).start()
        if first:
            own_right(2).start()
            own_left(2).start()
            cross(2, 0).start()

    pass_on(0, True)
    load_w[0].wait()
    load_w[1].wait()
    from_partner(0, 0).wait_recv()
    from_partner(1, 0).wait_recv()
    rows_here(0)
    gate_up(0, 0)
    pass_on(1, False)
    for p in range(2):
        for j in (1, 2):
            from_partner(p, j).wait_recv()

    @pl.loop(1, 3)
    def _(j):
        gate_up(0, j)

    rows_here(1)

    @pl.loop(0, 3)
    def _(j):
        gate_up(1, j)

    pass_on(2, False)
    for p in range(2):
        relay(p).wait_recv()
        cross(p, 3).start()
    rows_here(3)

    @pl.loop(0, 3)
    def _(j):
        gate_up(3, j)

    for p in range(2):
        from_partner(p, 3).wait_recv()
    for g in (0, 1, 3):
        gate_up(g, 3)
    rows_here(2)

    @pl.loop(0, 4)
    def _(j):
        gate_up(2, j)

    relay(2).wait_recv()
    cross(2, 3).start()
    load_w[2].wait()
    for j in range(SIDE):
        from_partner(2, j).wait_recv()

    def back(r):
        part = pl.ds(pl.multiple_of(r * cap, cap), cap)
        return remote(
            res.at[part, :], ret.at[part, :], back_s.at[r], back_r.at[r],
            peer(SIDE - r // SIDE, SIDE - r % SIDE), tp,
        )

    for g in (2, 1, 3, 0):
        rows = pl.ds(g * rows_g, rows_g)

        @pl.loop(0, tiles)
        def _(n):
            cols = pl.ds(pl.multiple_of(n * 256, 256), 256)
            w_tile = wd[:, :, cols].reshape(NTP * unit, 256)
            done = dot(act[rows, :], w_tile).astype(BF16)
            if g == 0:
                ret[0:cap, cols] = done[0:cap, :]
                res[cap:rows_g, cols] = done[cap:rows_g, :]
            else:
                res[rows, cols] = done

        for dx in (2, 1, 3, 0):
            if g or dx:
                back(g * SIDE + dx).start()

    for i, g in enumerate(GROUP_ORDER):
        for dx in range(SIDE):
            if g or dx:
                back(g * SIDE + dx).wait_recv()
        rows = pl.ds(g * rows_g, rows_g)

        @pl.loop(0, tiles)
        def _(n):
            cols = pl.ds(pl.multiple_of(n * 256, 256), 256)
            terms = dot(wmat[:, rows], ret[rows, cols])
            total = terms[0:toks] + terms[toks : 2 * toks] + terms[2 * toks : 3 * toks]
            if i == 0:
                comb[:, cols] = total
            else:
                comb[:, cols] += total

    @pl.loop(1, NTP)
    def _(k):
        og_copy(k, (tp + NTP - k) % NTP, (tp + k) % NTP).wait()

    @pl.loop(0, toks // 16)
    def _(i):
        strip = pl.ds(pl.multiple_of(i * 16, 16), 16)
        v = comb[strip, :]
        scale = lax.rsqrt(jnp.mean(v * v, axis=-1, keepdims=True) + EPS)
        for t in range(NTP):
            part = v[:, t * slice_w : (t + 1) * slice_w]
            mix[t, strip, :] = (part * scale * ogbuf[t]).astype(BF16)

    def fin(k, frm, to):
        at = pl.ds(pl.multiple_of(frm * toks, toks), toks)
        return remote(mix.at[to], out_hbm.at[at, :], fin_s.at[k], fin_r.at[k], ep, to)

    @pl.loop(1, NTP)
    def _(k):
        fin(k, tp, (tp + k) % NTP).start()

    keep = pltpu.make_async_copy(mix.at[tp], out_hbm.at[own, :], loc_sem.at[4])
    keep.start()

    for p in range(3):
        own_right(p).wait_send()
        own_left(p).wait_send()
        relay(p).wait_send()
        for j in range(SIDE):
            cross(p, j).wait_send()

    @pl.loop(1, NEP)
    def _(r):
        dispatch(r).wait_send()
        back(r).wait_send()

    @pl.loop(1, NTP)
    def _(k):
        fin(k, (tp + NTP - k) % NTP, (tp + k) % NTP).wait()

    keep.wait()


def local(tokens, expert_ids, gate_values, norm_gain, gate_weight, up_weight, down_weight, out_gain):
    toks, width = tokens.shape
    cap = toks // 2
    slots = NEP * cap
    unit = gate_weight.shape[2]
    hidden = NTP * unit
    slice_w = width // NTP
    vmem, hbm = pltpu.VMEM, pl.BlockSpec(memory_space=pl.ANY)
    in_vmem = pl.BlockSpec(memory_space=pltpu.VMEM)
    dma = pltpu.SemaphoreType.DMA
    return pl.pallas_call(
        kernel,
        out_shape=jax.ShapeDtypeStruct((NTP * toks, slice_w), BF16),
        in_specs=[hbm, in_vmem, in_vmem, in_vmem, hbm, hbm, hbm, in_vmem],
        out_specs=hbm,
        scratch_shapes=[
            vmem((toks, width), BF16),
            vmem((toks, width), BF16),
            vmem((slots, toks), BF16),
            vmem((NEP, toks), F32),
            vmem((NEP, toks), F32),
            vmem((slots, width), BF16),
            vmem((slots, width), BF16),
            vmem((NTP, width, unit), BF16),
            vmem((NTP, width, unit), BF16),
            vmem((NTP, unit, width), BF16),
            vmem((slots, hidden), BF16),
            vmem((slots, width), BF16),
            vmem((slots, width), BF16),
            vmem((3 * toks, slots), BF16),
            vmem((toks, width), F32),
            vmem((NTP, toks, slice_w), BF16),
            vmem((NTP, 1, slice_w), F32),
            dma((5,)), dma((3,)), dma((3,)), dma((3,)), dma((3, SIDE)), dma((3, 3)), dma((3, SIDE)),
            dma((NEP,)), dma((NEP,)), dma((NEP,)), dma((NEP,)),
            dma((NTP,)), dma((NTP,)), dma((NTP,)), dma((NTP,)),
        ],
        compiler_params=pltpu.CompilerParams(
            collective_id=0, has_side_effects=True, vmem_limit_bytes=60000 * 1024
        ),
    )(
        tokens, expert_ids.T, gate_values.T, norm_gain.reshape(1, width),
        gate_weight, up_weight, down_weight, out_gain.reshape(1, slice_w),
    )


def solution(mesh):
    in_specs = (
        P(("ep", "tp"), None), P("ep", None), P("ep", None), P(),
        P("ep", None, "tp"), P("ep", None, "tp"), P("ep", "tp", None), P("tp"),
    )
    return jax.shard_map(
        local, mesh=mesh, in_specs=in_specs, out_specs=P("ep", "tp"), check_vma=False
    )
```

```python
import jax
import jax.numpy as jnp
from jax import lax
from jax.experimental import pallas as pl
from jax.experimental.pallas import tpu as pltpu
from jax.sharding import PartitionSpec as P

MESH = pl.DeviceIdType.MESH
F32, BF16 = jnp.float32, jnp.bfloat16
EPS = 1e-05
LIMIT = 7.0
ALPHA = 1.702
SIDE = 4
NEP, NTP = 16, 8
ORDER = (
    ((3, 2), (3, 3), (2, 3), (1, 1), (1, 0), (3, 0), (2, 1), (3, 1), (1, 3), (0, 2), (2, 2), (0, 1), (0, 3), (1, 2), (2, 0), (0, 0)),
    ((2, 2), (1, 1), (3, 3), (0, 1), (0, 3), (1, 3), (3, 1), (2, 1), (2, 3), (3, 2), (1, 0), (3, 0), (2, 0), (1, 2), (0, 2), (0, 0)),
)
SELF = NEP - 1


def dot(a, b):
    return jnp.dot(a, b, preferred_element_type=F32)


def kernel(
    tok_hbm, ids_ref, gates_ref, ngain_ref, wg_hbm, wu_hbm, wd_hbm, ogain_ref, out_hbm,
    tok, normed, pbuf, vref, gref, snd, xbuf, wg, wu, wd, act, res, ret, wmat, comb, mix, ogbuf,
    loc_sem, wl_s, wr_s, wy_s, wc_s, wi_r, wc_r, disp_s, disp_r, back_s, back_r, fin_s, fin_r, og_s, og_r,
):
    toks, width = tok.shape
    cap = toks // 2
    rows_g = SIDE * cap
    unit = wg.shape[2]
    slice_w = mix.shape[2]
    tiles = width // 256

    ep = lax.axis_index("ep")
    tp = lax.axis_index("tp")
    z, x = ep // SIDE, ep % SIDE
    y, core = tp // 2, tp % 2

    def peer(dz, dx):
        return ((z + dz) % SIDE) * SIDE + (x + dx) % SIDE

    def offset(p, sign):
        (z0, x0), (z1, x1) = ORDER[0][p], ORDER[1][p]
        dz, dx = z0 + core * (z1 - z0), x0 + core * (x1 - x0)
        return peer(dz, dx) if sign > 0 else peer(SIDE - dz, SIDE - dx)

    right = ((y + 1) % SIDE) * 2 + core
    left = ((y + SIDE - 1) % SIDE) * 2 + core
    partner = y * 2 + 1 - core

    barrier = pltpu.get_barrier_semaphore()

    @pl.loop(1, NEP)
    def _(r):
        pl.semaphore_signal(
            barrier, inc=1, device_id=(peer(r // SIDE, r % SIDE), tp), device_id_type=MESH
        )

    @pl.loop(1, NTP)
    def _(k):
        pl.semaphore_signal(barrier, inc=1, device_id=(ep, (tp + k) % NTP), device_id_type=MESH)

    load_tok = pltpu.make_async_copy(tok_hbm, tok, loc_sem.at[0])
    load_tok.start()
    bufs = (wg, wu, wd)
    srcs = (wg_hbm.at[0], wu_hbm.at[0], wd_hbm.at[0])
    load_w = [
        pltpu.make_async_copy(srcs[p], bufs[p].at[core], loc_sem.at[1 + p]) for p in range(3)
    ]
    for cp in load_w:
        cp.start()

    def remote(src, dst, send, recv, ep_to, tp_to):
        return pltpu.make_async_remote_copy(
            src_ref=src, dst_ref=dst, send_sem=send, recv_sem=recv,
            device_id=(ep_to, tp_to), device_id_type=MESH,
        )

    def own_right(p):
        return remote(srcs[p], bufs[p].at[2 + core], wr_s.at[p], wi_r.at[p, 0], ep, right)

    def own_left(p):
        return remote(srcs[p], bufs[p].at[4 + core], wl_s.at[p], wi_r.at[p, 1], ep, left)

    def relay(p):
        return remote(
            bufs[p].at[2 + 2 * core + core], bufs[p].at[6 + core], wy_s.at[p], wi_r.at[p, 2],
            ep, right + core * (left - right),
        )

    def cross(p, j):
        src = srcs[p] if j == 0 else bufs[p].at[2 * j + core]
        return remote(src, bufs[p].at[2 * j + core], wc_s.at[p, j], wc_r.at[p, j], ep, partner)

    def from_partner(p, j):
        slot = bufs[p].at[2 * j + 1 - core]
        return remote(slot, slot, wc_s.at[p, j], wc_r.at[p, j], ep, partner)

    own = pl.ds(pl.multiple_of(tp * toks, toks), toks)
    ids = ids_ref[:, own]
    gates = gates_ref[:, own]
    place = lax.broadcasted_iota(jnp.int32, (NEP, toks), 0)
    expert = jnp.zeros((NEP, toks), jnp.int32)
    for p in range(NEP):
        expert = jnp.where(place == p, offset(p, 1), expert)
    named = jnp.zeros((NEP, toks), F32)
    gate_of = jnp.zeros((NEP, toks), F32)
    for k in range(ids.shape[0]):
        hit = ids[k : k + 1, :] == expert
        named = jnp.where(hit, 1.0, named)
        gate_of = jnp.where(hit, gates[k : k + 1, :], gate_of)
    t_from = lax.broadcasted_iota(jnp.int32, (toks, toks), 0)
    t_to = lax.broadcasted_iota(jnp.int32, (toks, toks), 1)
    earlier = jnp.where(t_from < t_to, 1.0, 0.0).astype(BF16)
    slot = dot(named.astype(BF16), earlier)
    vref[...] = jnp.where(named > 0.0, slot, -1.0)
    gref[...] = gate_of
    slot_iota = lax.broadcasted_iota(jnp.int32, (cap, toks), 0).astype(F32)

    @pl.loop(0, NEP)
    def _(r):
        pick = jnp.where(vref[pl.ds(r, 1), :] == slot_iota, 1.0, 0.0)
        pbuf[pl.ds(pl.multiple_of(r * cap, cap), cap), :] = pick.astype(BF16)

    load_tok.wait()
    ngain = ngain_ref[...]

    @pl.loop(0, toks // 16)
    def _(i):
        strip = pl.ds(pl.multiple_of(i * 16, 16), 16)
        v = tok[strip, :].astype(F32)
        ms = jnp.mean(v * v, axis=-1, keepdims=True)
        normed[strip, :] = (v * lax.rsqrt(ms + EPS) * ngain).astype(BF16)

    pl.semaphore_wait(barrier, NEP - 1 + NTP - 1)
    for p in range(2):
        own_right(p).start()
        own_left(p).start()
    for p in range(2):
        cross(p, 0).start()

    ogbuf[tp] = ogain_ref[...]

    def og_copy(k, frm, to):
        return remote(ogain_ref, ogbuf.at[frm], og_s.at[k], og_r.at[k], ep, to)

    @pl.loop(1, NTP)
    def _(k):
        og_copy(k, tp, (tp + k) % NTP).start()

    def dispatch(p, to):
        part = pl.ds(pl.multiple_of(p * cap, cap), cap)
        return remote(snd.at[part, :], xbuf.at[part, :], disp_s.at[p], disp_r.at[p], to, tp)

    for g in range(SIDE):
        group = pl.ds(g * rows_g, rows_g)

        @pl.loop(0, tiles)
        def _(n):
            cols = pl.ds(pl.multiple_of(n * 256, 256), 256)
            picked = dot(pbuf[group, :], normed[:, cols]).astype(BF16)
            snd[group, cols] = picked
            if g == SIDE - 1:
                xbuf[SELF * cap :, cols] = picked[rows_g - cap :, :]

        for p in range(g * SIDE, (g + 1) * SIDE):
            if p != SELF:
                dispatch(p, offset(p, 1)).start()

    @pl.loop(0, NEP // 2)
    def _(q):
        halves = [
            jnp.where(
                vref[pl.ds(2 * q + h, 1), :] == slot_iota, gref[pl.ds(2 * q + h, 1), :], 0.0
            )
            for h in range(2)
        ]
        w = jnp.concatenate(halves, axis=0).T
        cols = pl.ds(pl.multiple_of(q * 2 * cap, 2 * cap), 2 * cap)
        for s in range(3):
            term = w.astype(BF16)
            wmat[s * toks : (s + 1) * toks, cols] = term
            w = w - term.astype(F32)

    def gate_up(g, j):
        rows = pl.ds(pl.multiple_of(g * rows_g, rows_g), rows_g)
        xg = xbuf[rows, :]
        gate_part = dot(xg, jnp.concatenate([wg[2 * j], wg[2 * j + 1]], axis=1))
        up_part = dot(xg, jnp.concatenate([wu[2 * j], wu[2 * j + 1]], axis=1))
        gl = jnp.minimum(gate_part, LIMIT)
        li = jnp.clip(up_part, -LIMIT, LIMIT)
        fresh = gl * jax.nn.sigmoid(ALPHA * gl) * (li + 1.0)
        act[rows, pl.ds(pl.multiple_of(j * 2 * unit, 2 * unit), 2 * unit)] = fresh.astype(BF16)

    def rows_here(g):
        for p in range(g * SIDE, (g + 1) * SIDE):
            if p != SELF:
                dispatch(p, partner).wait_recv()

    def pass_on(p, first):
        own_right(p).wait_recv()
        own_left(p).wait_recv()
        relay(p).start()
        cross(p, 1).start()
        cross(p, 2).start()
        if first:
            own_right(2).start()
            own_left(2).start()
            cross(2, 0).start()

    pass_on(0, True)
    load_w[0].wait()
    load_w[1].wait()
    from_partner(0, 0).wait_recv()
    from_partner(1, 0).wait_recv()
    rows_here(0)
    gate_up(0, 0)
    pass_on(1, False)
    for p in range(2):
        for j in (1, 2):
            from_partner(p, j).wait_recv()

    @pl.loop(1, 3)
    def _(j):
        gate_up(0, j)

    rows_here(1)

    @pl.loop(0, 3)
    def _(j):
        gate_up(1, j)

    pass_on(2, False)
    for p in range(2):
        relay(p).wait_recv()
        cross(p, 3).start()
    rows_here(2)

    @pl.loop(0, 3)
    def _(j):
        gate_up(2, j)

    for p in range(2):
        from_partner(p, 3).wait_recv()

    @pl.loop(0, 3)
    def _(g):
        gate_up(g, 3)

    rows_here(3)

    @pl.loop(0, 4)
    def _(j):
        gate_up(3, j)

    relay(2).wait_recv()
    cross(2, 3).start()
    load_w[2].wait()
    for j in range(SIDE):
        from_partner(2, j).wait_recv()

    def back(p, to):
        part = pl.ds(pl.multiple_of(p * cap, cap), cap)
        return remote(res.at[part, :], ret.at[part, :], back_s.at[p], back_r.at[p], to, tp)

    for g in range(SIDE):
        rows = pl.ds(g * rows_g, rows_g)

        @pl.loop(0, tiles)
        def _(n):
            cols = pl.ds(pl.multiple_of(n * 256, 256), 256)
            w_tile = wd[:, :, cols].reshape(NTP * unit, 256)
            done = dot(act[rows, :], w_tile).astype(BF16)
            res[rows, cols] = done
            if g == SIDE - 1:
                ret[SELF * cap :, cols] = done[rows_g - cap :, :]

        for p in range(g * SIDE, (g + 1) * SIDE):
            if p != SELF:
                back(p, offset(p, -1)).start()

    for g in range(SIDE):
        for p in range(g * SIDE, (g + 1) * SIDE):
            if p != SELF:
                back(p, partner).wait_recv()
        rows = pl.ds(g * rows_g, rows_g)

        @pl.loop(0, tiles)
        def _(n):
            cols = pl.ds(pl.multiple_of(n * 256, 256), 256)
            terms = dot(wmat[:, rows], ret[rows, cols])
            total = terms[0:toks] + terms[toks : 2 * toks] + terms[2 * toks : 3 * toks]
            if g == 0:
                comb[:, cols] = total
            else:
                comb[:, cols] += total

    @pl.loop(1, NTP)
    def _(k):
        og_copy(k, (tp + NTP - k) % NTP, (tp + k) % NTP).wait()

    @pl.loop(0, toks // 16)
    def _(i):
        strip = pl.ds(pl.multiple_of(i * 16, 16), 16)
        v = comb[strip, :]
        scale = lax.rsqrt(jnp.mean(v * v, axis=-1, keepdims=True) + EPS)
        for t in range(NTP):
            part = v[:, t * slice_w : (t + 1) * slice_w]
            mix[t, strip, :] = (part * scale * ogbuf[t]).astype(BF16)

    def fin(k, frm, to):
        at = pl.ds(pl.multiple_of(frm * toks, toks), toks)
        return remote(mix.at[to], out_hbm.at[at, :], fin_s.at[k], fin_r.at[k], ep, to)

    @pl.loop(1, NTP)
    def _(k):
        fin(k, tp, (tp + k) % NTP).start()

    keep = pltpu.make_async_copy(mix.at[tp], out_hbm.at[own, :], loc_sem.at[4])
    keep.start()

    for p in range(3):
        own_right(p).wait_send()
        own_left(p).wait_send()
        relay(p).wait_send()
        for j in range(SIDE):
            cross(p, j).wait_send()

    @pl.loop(0, SELF)
    def _(p):
        dispatch(p, partner).wait_send()
        back(p, partner).wait_send()

    @pl.loop(1, NTP)
    def _(k):
        fin(k, (tp + NTP - k) % NTP, (tp + k) % NTP).wait()

    keep.wait()


def local(tokens, expert_ids, gate_values, norm_gain, gate_weight, up_weight, down_weight, out_gain):
    toks, width = tokens.shape
    cap = toks // 2
    slots = NEP * cap
    unit = gate_weight.shape[2]
    hidden = NTP * unit
    slice_w = width // NTP
    vmem, hbm = pltpu.VMEM, pl.BlockSpec(memory_space=pl.ANY)
    in_vmem = pl.BlockSpec(memory_space=pltpu.VMEM)
    dma = pltpu.SemaphoreType.DMA
    return pl.pallas_call(
        kernel,
        out_shape=jax.ShapeDtypeStruct((NTP * toks, slice_w), BF16),
        in_specs=[hbm, in_vmem, in_vmem, in_vmem, hbm, hbm, hbm, in_vmem],
        out_specs=hbm,
        scratch_shapes=[
            vmem((toks, width), BF16),
            vmem((toks, width), BF16),
            vmem((slots, toks), BF16),
            vmem((NEP, toks), F32),
            vmem((NEP, toks), F32),
            vmem((slots, width), BF16),
            vmem((slots, width), BF16),
            vmem((NTP, width, unit), BF16),
            vmem((NTP, width, unit), BF16),
            vmem((NTP, unit, width), BF16),
            vmem((slots, hidden), BF16),
            vmem((slots, width), BF16),
            vmem((slots, width), BF16),
            vmem((3 * toks, slots), BF16),
            vmem((toks, width), F32),
            vmem((NTP, toks, slice_w), BF16),
            vmem((NTP, 1, slice_w), F32),
            dma((5,)), dma((3,)), dma((3,)), dma((3,)), dma((3, SIDE)), dma((3, 3)), dma((3, SIDE)),
            dma((NEP,)), dma((NEP,)), dma((NEP,)), dma((NEP,)),
            dma((NTP,)), dma((NTP,)), dma((NTP,)), dma((NTP,)),
        ],
        compiler_params=pltpu.CompilerParams(
            collective_id=0, has_side_effects=True, vmem_limit_bytes=60000 * 1024
        ),
    )(
        tokens, expert_ids.T, gate_values.T, norm_gain.reshape(1, width),
        gate_weight, up_weight, down_weight, out_gain.reshape(1, slice_w),
    )


def solution(mesh):
    in_specs = (
        P(("ep", "tp"), None), P("ep", None), P("ep", None), P(),
        P("ep", None, "tp"), P("ep", None, "tp"), P("ep", "tp", None), P("tp"),
    )
    return jax.shard_map(
        local, mesh=mesh, in_specs=in_specs, out_specs=P("ep", "tp"), check_vma=False
    )
```

```python
import jax
import jax.numpy as jnp
from jax import lax
from jax.experimental import pallas as pl
from jax.experimental.pallas import tpu as pltpu
from jax.sharding import PartitionSpec as P

MESH = pl.DeviceIdType.MESH
F32, BF16 = jnp.float32, jnp.bfloat16
EPS = 1e-05
LIMIT = 7.0
ALPHA = 1.702
SIDE = 4
NEP, NTP = 16, 8
SENT = (1, 3, 2, 0)


def dot(a, b):
    return jnp.dot(a, b, preferred_element_type=F32)


def kernel(
    tok_hbm, ids_ref, gates_ref, ngain_ref, wg_hbm, wu_hbm, wd_hbm, ogain_ref, out_hbm,
    tok, normed, pbuf, vref, gref, snd, xbuf, mid, wg, wu, wd, act, res, ret, mid_back, wmat, comb, mix, ogbuf,
    loc_sem, wl_s, wr_s, wy_s, wc_s, wi_r, wc_r, a_s, a_r, b_s, b_r, c_s, c_r, d_s, d_r, fin_s, fin_r, og_s, og_r,
):
    toks, width = tok.shape
    cap = toks // 2
    rows_g = SIDE * cap
    unit = wg.shape[2]
    slice_w = mix.shape[2]
    tiles = width // 256

    ep = lax.axis_index("ep")
    tp = lax.axis_index("tp")
    z, x = ep // SIDE, ep % SIDE
    y, core = tp // 2, tp % 2

    def peer(dz, dx):
        return ((z + dz) % SIDE) * SIDE + (x + dx) % SIDE

    def offset(a, b):
        return peer(core * a + (1 - core) * b, (1 - core) * a + core * b)

    right = ((y + 1) % SIDE) * 2 + core
    left = ((y + SIDE - 1) % SIDE) * 2 + core
    partner = y * 2 + 1 - core

    barrier = pltpu.get_barrier_semaphore()

    @pl.loop(1, SIDE)
    def _(r):
        for to in (peer(r, 0), peer(0, r)):
            pl.semaphore_signal(barrier, inc=1, device_id=(to, tp), device_id_type=MESH)

    @pl.loop(1, NTP)
    def _(k):
        pl.semaphore_signal(barrier, inc=1, device_id=(ep, (tp + k) % NTP), device_id_type=MESH)

    load_tok = pltpu.make_async_copy(tok_hbm, tok, loc_sem.at[0])
    load_tok.start()
    bufs = (wg, wu, wd)
    srcs = (wg_hbm.at[0], wu_hbm.at[0], wd_hbm.at[0])
    load_w = [
        pltpu.make_async_copy(srcs[p], bufs[p].at[core], loc_sem.at[1 + p]) for p in range(3)
    ]
    for cp in load_w:
        cp.start()

    def remote(src, dst, send, recv, ep_to, tp_to):
        return pltpu.make_async_remote_copy(
            src_ref=src, dst_ref=dst, send_sem=send, recv_sem=recv,
            device_id=(ep_to, tp_to), device_id_type=MESH,
        )

    def own_right(p):
        return remote(srcs[p], bufs[p].at[2 + core], wr_s.at[p], wi_r.at[p, 0], ep, right)

    def own_left(p):
        return remote(srcs[p], bufs[p].at[4 + core], wl_s.at[p], wi_r.at[p, 1], ep, left)

    def relay(p):
        return remote(
            bufs[p].at[2 + 2 * core + core], bufs[p].at[6 + core], wy_s.at[p], wi_r.at[p, 2],
            ep, right + core * (left - right),
        )

    def cross(p, j):
        src = srcs[p] if j == 0 else bufs[p].at[2 * j + core]
        return remote(src, bufs[p].at[2 * j + core], wc_s.at[p, j], wc_r.at[p, j], ep, partner)

    def from_partner(p, j):
        slot = bufs[p].at[2 * j + 1 - core]
        return remote(slot, slot, wc_s.at[p, j], wc_r.at[p, j], ep, partner)

    own = pl.ds(pl.multiple_of(tp * toks, toks), toks)
    ids = ids_ref[:, own]
    gates = gates_ref[:, own]
    place = lax.broadcasted_iota(jnp.int32, (NEP, toks), 0)
    expert = jnp.zeros((NEP, toks), jnp.int32)
    for p in range(NEP):
        expert = jnp.where(place == p, offset(p // SIDE, p % SIDE), expert)
    named = jnp.zeros((NEP, toks), F32)
    gate_of = jnp.zeros((NEP, toks), F32)
    for k in range(ids.shape[0]):
        hit = ids[k : k + 1, :] == expert
        named = jnp.where(hit, 1.0, named)
        gate_of = jnp.where(hit, gates[k : k + 1, :], gate_of)
    t_from = lax.broadcasted_iota(jnp.int32, (toks, toks), 0)
    t_to = lax.broadcasted_iota(jnp.int32, (toks, toks), 1)
    earlier = jnp.where(t_from < t_to, 1.0, 0.0).astype(BF16)
    slot = dot(named.astype(BF16), earlier)
    vref[...] = jnp.where(named > 0.0, slot, -1.0)
    gref[...] = gate_of
    slot_iota = lax.broadcasted_iota(jnp.int32, (cap, toks), 0).astype(F32)

    @pl.loop(0, NEP)
    def _(r):
        pick = jnp.where(vref[pl.ds(r, 1), :] == slot_iota, 1.0, 0.0)
        pbuf[pl.ds(pl.multiple_of(r * cap, cap), cap), :] = pick.astype(BF16)

    load_tok.wait()
    ngain = ngain_ref[...]

    @pl.loop(0, toks // 16)
    def _(i):
        strip = pl.ds(pl.multiple_of(i * 16, 16), 16)
        v = tok[strip, :].astype(F32)
        ms = jnp.mean(v * v, axis=-1, keepdims=True)
        normed[strip, :] = (v * lax.rsqrt(ms + EPS) * ngain).astype(BF16)

    pl.semaphore_wait(barrier, 2 * (SIDE - 1) + NTP - 1)
    for p in range(2):
        own_right(p).start()
        own_left(p).start()
    for p in range(2):
        cross(p, 0).start()

    ogbuf[tp] = ogain_ref[...]

    def og_copy(k, frm, to):
        return remote(ogain_ref, ogbuf.at[frm], og_s.at[k], og_r.at[k], ep, to)

    @pl.loop(1, NTP)
    def _(k):
        og_copy(k, tp, (tp + k) % NTP).start()

    class Exchange:
        def __init__(self, src, via, dst, sems, sign):
            self.src, self.via, self.dst, self.sems, self.sign = src, via, dst, sems, sign

        def to(self, a, b):
            return offset(a, b) if self.sign > 0 else offset((SIDE - a) % SIDE, (SIDE - b) % SIDE)

        def first(self, a, stays):
            part = pl.ds(a * rows_g, cap) if stays else pl.ds(a * rows_g + cap, rows_g - cap)
            dst = self.dst.at[part, :] if stays else self.via.at[a - 1]
            s_sem, r_sem = self.sems[0].at[a, stays], self.sems[1].at[a, stays]
            return remote(self.src.at[part, :], dst, s_sem, r_sem, self.to(a, 0), tp)

        def second(self, a, b):
            part = pl.ds(a * rows_g + b * cap, cap)
            src = self.via.at[a - 1, pl.ds((b - 1) * cap, cap), :] if a else self.src.at[part, :]
            return remote(src, self.dst.at[part, :], self.sems[2].at[a, b], self.sems[3].at[a, b], self.to(0, b), tp)

        def send(self, a):
            if a:
                for stays in range(2):
                    self.first(a, stays).start()
            else:
                for b in (2, 1, 3):
                    self.second(0, b).start()

        def forward(self, a):
            self.first(a, 0).wait_recv()
            for b in (2, 1, 3):
                self.second(a, b).start()

        def here(self, a):
            if a:
                self.first(a, 1).wait_recv()
            for b in (1, 3, 2):
                self.second(a, b).wait_recv()

        def drain(self):
            for a in range(SIDE):
                if a:
                    for stays in range(2):
                        self.first(a, stays).wait_send()
                for b in range(1, SIDE):
                    self.second(a, b).wait_send()

    out = Exchange(snd, mid, xbuf, (a_s, a_r, b_s, b_r), 1)
    back = Exchange(res, mid_back, ret, (c_s, c_r, d_s, d_r), -1)

    for a in SENT:
        group = pl.ds(a * rows_g, rows_g)

        @pl.loop(0, tiles)
        def _(n):
            cols = pl.ds(pl.multiple_of(n * 256, 256), 256)
            picked = dot(pbuf[group, :], normed[:, cols]).astype(BF16)
            snd[group, cols] = picked
            if a == 0:
                xbuf[0:cap, cols] = picked[0:cap, :]

        out.send(a)

    @pl.loop(0, NEP // 2)
    def _(q):
        halves = [
            jnp.where(
                vref[pl.ds(2 * q + h, 1), :] == slot_iota, gref[pl.ds(2 * q + h, 1), :], 0.0
            )
            for h in range(2)
        ]
        w = jnp.concatenate(halves, axis=0).T
        cols = pl.ds(pl.multiple_of(q * 2 * cap, 2 * cap), 2 * cap)
        for s in range(3):
            term = w.astype(BF16)
            wmat[s * toks : (s + 1) * toks, cols] = term
            w = w - term.astype(F32)

    def gate_up(g, j):
        rows = pl.ds(pl.multiple_of(g * rows_g, rows_g), rows_g)
        xg = xbuf[rows, :]
        gate_part = dot(xg, jnp.concatenate([wg[2 * j], wg[2 * j + 1]], axis=1))
        up_part = dot(xg, jnp.concatenate([wu[2 * j], wu[2 * j + 1]], axis=1))
        gl = jnp.minimum(gate_part, LIMIT)
        li = jnp.clip(up_part, -LIMIT, LIMIT)
        fresh = gl * jax.nn.sigmoid(ALPHA * gl) * (li + 1.0)
        act[rows, pl.ds(pl.multiple_of(j * 2 * unit, 2 * unit), 2 * unit)] = fresh.astype(BF16)

    def pass_on(p, first):
        own_right(p).wait_recv()
        own_left(p).wait_recv()
        relay(p).start()
        cross(p, 1).start()
        cross(p, 2).start()
        if first:
            own_right(2).start()
            own_left(2).start()
            cross(2, 0).start()

    pass_on(0, True)
    out.forward(1)
    out.forward(3)
    load_w[0].wait()
    load_w[1].wait()
    from_partner(0, 0).wait_recv()
    from_partner(1, 0).wait_recv()
    out.here(0)
    gate_up(0, 0)
    pass_on(1, False)
    out.forward(2)
    for p in range(2):
        for j in (1, 2):
            from_partner(p, j).wait_recv()

    @pl.loop(1, 3)
    def _(j):
        gate_up(0, j)

    out.here(1)

    @pl.loop(0, 3)
    def _(j):
        gate_up(1, j)

    pass_on(2, False)
    for p in range(2):
        relay(p).wait_recv()
        cross(p, 3).start()
    out.here(3)

    @pl.loop(0, 3)
    def _(j):
        gate_up(3, j)

    for p in range(2):
        from_partner(p, 3).wait_recv()
    gate_up(1, 3)
    gate_up(3, 3)
    gate_up(0, 3)
    out.here(2)

    @pl.loop(0, SIDE)
    def _(j):
        gate_up(2, j)

    relay(2).wait_recv()
    cross(2, 3).start()
    load_w[2].wait()
    for j in range(SIDE):
        from_partner(2, j).wait_recv()

    for a in SENT:
        rows = pl.ds(a * rows_g, rows_g)

        @pl.loop(0, tiles)
        def _(n):
            cols = pl.ds(pl.multiple_of(n * 256, 256), 256)
            w_tile = wd[:, :, cols].reshape(NTP * unit, 256)
            done = dot(act[rows, :], w_tile).astype(BF16)
            res[rows, cols] = done
            if a == 0:
                ret[0:cap, cols] = done[0:cap, :]

        back.send(a)

    for a in SENT[:-1]:
        back.forward(a)

    for g in (0, 1, 3, 2):
        back.here(g)
        rows = pl.ds(g * rows_g, rows_g)

        @pl.loop(0, tiles)
        def _(n):
            cols = pl.ds(pl.multiple_of(n * 256, 256), 256)
            terms = dot(wmat[:, rows], ret[rows, cols])
            total = terms[0:toks] + terms[toks : 2 * toks] + terms[2 * toks : 3 * toks]
            if g == 0:
                comb[:, cols] = total
            else:
                comb[:, cols] += total

    @pl.loop(1, NTP)
    def _(k):
        og_copy(k, (tp + NTP - k) % NTP, (tp + k) % NTP).wait()

    @pl.loop(0, toks // 16)
    def _(i):
        strip = pl.ds(pl.multiple_of(i * 16, 16), 16)
        v = comb[strip, :]
        scale = lax.rsqrt(jnp.mean(v * v, axis=-1, keepdims=True) + EPS)
        for t in range(NTP):
            part = v[:, t * slice_w : (t + 1) * slice_w]
            mix[t, strip, :] = (part * scale * ogbuf[t]).astype(BF16)

    def fin(k, frm, to):
        at = pl.ds(pl.multiple_of(frm * toks, toks), toks)
        return remote(mix.at[to], out_hbm.at[at, :], fin_s.at[k], fin_r.at[k], ep, to)

    @pl.loop(1, NTP)
    def _(k):
        fin(k, tp, (tp + k) % NTP).start()

    keep = pltpu.make_async_copy(mix.at[tp], out_hbm.at[own, :], loc_sem.at[4])
    keep.start()

    for p in range(3):
        own_right(p).wait_send()
        own_left(p).wait_send()
        relay(p).wait_send()
        for j in range(SIDE):
            cross(p, j).wait_send()

    out.drain()
    back.drain()

    @pl.loop(1, NTP)
    def _(k):
        fin(k, (tp + NTP - k) % NTP, (tp + k) % NTP).wait()

    keep.wait()


def local(tokens, expert_ids, gate_values, norm_gain, gate_weight, up_weight, down_weight, out_gain):
    toks, width = tokens.shape
    cap = toks // 2
    slots = NEP * cap
    unit = gate_weight.shape[2]
    hidden = NTP * unit
    slice_w = width // NTP
    vmem, hbm = pltpu.VMEM, pl.BlockSpec(memory_space=pl.ANY)
    in_vmem = pl.BlockSpec(memory_space=pltpu.VMEM)
    dma = pltpu.SemaphoreType.DMA
    return pl.pallas_call(
        kernel,
        out_shape=jax.ShapeDtypeStruct((NTP * toks, slice_w), BF16),
        in_specs=[hbm, in_vmem, in_vmem, in_vmem, hbm, hbm, hbm, in_vmem],
        out_specs=hbm,
        scratch_shapes=[
            vmem((toks, width), BF16),
            vmem((toks, width), BF16),
            vmem((slots, toks), BF16),
            vmem((NEP, toks), F32),
            vmem((NEP, toks), F32),
            vmem((slots, width), BF16),
            vmem((slots, width), BF16),
            vmem((SIDE - 1, 3 * cap, width), BF16),
            vmem((NTP, width, unit), BF16),
            vmem((NTP, width, unit), BF16),
            vmem((NTP, unit, width), BF16),
            vmem((slots, hidden), BF16),
            vmem((slots, width), BF16),
            vmem((slots, width), BF16),
            vmem((SIDE - 1, 3 * cap, width), BF16),
            vmem((3 * toks, slots), BF16),
            vmem((toks, width), F32),
            vmem((NTP, toks, slice_w), BF16),
            vmem((NTP, 1, slice_w), F32),
            dma((5,)), dma((3,)), dma((3,)), dma((3,)), dma((3, SIDE)), dma((3, 3)), dma((3, SIDE)),
            dma((SIDE, 2)), dma((SIDE, 2)), dma((SIDE, SIDE)), dma((SIDE, SIDE)),
            dma((SIDE, 2)), dma((SIDE, 2)), dma((SIDE, SIDE)), dma((SIDE, SIDE)),
            dma((NTP,)), dma((NTP,)), dma((NTP,)), dma((NTP,)),
        ],
        compiler_params=pltpu.CompilerParams(
            collective_id=0, has_side_effects=True, vmem_limit_bytes=60000 * 1024
        ),
    )(
        tokens, expert_ids.T, gate_values.T, norm_gain.reshape(1, width),
        gate_weight, up_weight, down_weight, out_gain.reshape(1, slice_w),
    )


def solution(mesh):
    in_specs = (
        P(("ep", "tp"), None), P("ep", None), P("ep", None), P(),
        P("ep", None, "tp"), P("ep", None, "tp"), P("ep", "tp", None), P("tp"),
    )
    return jax.shard_map(
        local, mesh=mesh, in_specs=in_specs, out_specs=P("ep", "tp"), check_vma=False
    )
```

```python
import jax
import jax.numpy as jnp
from jax import lax
from jax.experimental import pallas as pl
from jax.experimental.pallas import tpu as pltpu
from jax.sharding import PartitionSpec as P

MESH = pl.DeviceIdType.MESH
F32, BF16 = jnp.float32, jnp.bfloat16
EPS = 1e-05
LIMIT = 7.0
ALPHA = 1.702
SIDE = 4
NEP, NTP = 16, 8
SENT = (1, 3, 2, 0)


def dot(a, b):
    return jnp.dot(a, b, preferred_element_type=F32)


def kernel(
    tok_hbm, ids_ref, gates_ref, ngain_ref, wg_hbm, wu_hbm, wd_hbm, ogain_ref, out_hbm,
    tok, normed, pbuf, vref, gref, snd, xbuf, mid, wg, wu, wd, act, res, ret, mid_back, wmat, comb, mix, ogbuf,
    loc_sem, wl_s, wr_s, wy_s, wc_s, wi_r, wc_r, a_s, a_r, b_s, b_r, c_s, c_r, d_s, d_r, fin_s, fin_r, og_s, og_r,
):
    toks, width = tok.shape
    cap = toks // 2
    rows_g = SIDE * cap
    unit = wg.shape[2]
    slice_w = mix.shape[2]
    tiles = width // 256

    ep = lax.axis_index("ep")
    tp = lax.axis_index("tp")
    z, x = ep // SIDE, ep % SIDE
    y, core = tp // 2, tp % 2

    def peer(dz, dx):
        return ((z + dz) % SIDE) * SIDE + (x + dx) % SIDE

    def offset(a, b):
        return peer(core * a + (1 - core) * b, (1 - core) * a + core * b)

    right = ((y + 1) % SIDE) * 2 + core
    left = ((y + SIDE - 1) % SIDE) * 2 + core
    partner = y * 2 + 1 - core

    barrier = pltpu.get_barrier_semaphore()

    @pl.loop(1, SIDE)
    def _(r):
        for to in (peer(r, 0), peer(0, r)):
            pl.semaphore_signal(barrier, inc=1, device_id=(to, tp), device_id_type=MESH)

    @pl.loop(1, NTP)
    def _(k):
        pl.semaphore_signal(barrier, inc=1, device_id=(ep, (tp + k) % NTP), device_id_type=MESH)

    load_tok = pltpu.make_async_copy(tok_hbm, tok, loc_sem.at[0])
    load_tok.start()
    bufs = (wg, wu, wd)
    srcs = (wg_hbm.at[0], wu_hbm.at[0], wd_hbm.at[0])
    load_w = [
        pltpu.make_async_copy(srcs[p], bufs[p].at[core], loc_sem.at[1 + p]) for p in range(3)
    ]
    for cp in load_w:
        cp.start()

    def remote(src, dst, send, recv, ep_to, tp_to):
        return pltpu.make_async_remote_copy(
            src_ref=src, dst_ref=dst, send_sem=send, recv_sem=recv,
            device_id=(ep_to, tp_to), device_id_type=MESH,
        )

    def own_right(p):
        return remote(srcs[p], bufs[p].at[2 + core], wr_s.at[p], wi_r.at[p, 0], ep, right)

    def own_left(p):
        return remote(srcs[p], bufs[p].at[4 + core], wl_s.at[p], wi_r.at[p, 1], ep, left)

    def relay(p):
        return remote(
            bufs[p].at[2 + 2 * core + core], bufs[p].at[6 + core], wy_s.at[p], wi_r.at[p, 2],
            ep, right + core * (left - right),
        )

    def cross(p, j):
        src = srcs[p] if j == 0 else bufs[p].at[2 * j + core]
        return remote(src, bufs[p].at[2 * j + core], wc_s.at[p, j], wc_r.at[p, j], ep, partner)

    def from_partner(p, j):
        slot = bufs[p].at[2 * j + 1 - core]
        return remote(slot, slot, wc_s.at[p, j], wc_r.at[p, j], ep, partner)

    own = pl.ds(pl.multiple_of(tp * toks, toks), toks)
    ids = ids_ref[:, own]
    gates = gates_ref[:, own]
    place = lax.broadcasted_iota(jnp.int32, (NEP, toks), 0)
    expert = jnp.zeros((NEP, toks), jnp.int32)
    for p in range(NEP):
        expert = jnp.where(place == p, offset(p // SIDE, p % SIDE), expert)
    named = jnp.zeros((NEP, toks), F32)
    gate_of = jnp.zeros((NEP, toks), F32)
    for k in range(ids.shape[0]):
        hit = ids[k : k + 1, :] == expert
        named = jnp.where(hit, 1.0, named)
        gate_of = jnp.where(hit, gates[k : k + 1, :], gate_of)
    t_from = lax.broadcasted_iota(jnp.int32, (toks, toks), 0)
    t_to = lax.broadcasted_iota(jnp.int32, (toks, toks), 1)
    earlier = jnp.where(t_from < t_to, 1.0, 0.0).astype(BF16)
    slot = dot(named.astype(BF16), earlier)
    vref[...] = jnp.where(named > 0.0, slot, -1.0)
    gref[...] = gate_of
    slot_iota = lax.broadcasted_iota(jnp.int32, (cap, toks), 0).astype(F32)

    @pl.loop(0, NEP)
    def _(r):
        pick = jnp.where(vref[pl.ds(r, 1), :] == slot_iota, 1.0, 0.0)
        pbuf[pl.ds(pl.multiple_of(r * cap, cap), cap), :] = pick.astype(BF16)

    load_tok.wait()
    ngain = ngain_ref[...]

    @pl.loop(0, toks // 16)
    def _(i):
        strip = pl.ds(pl.multiple_of(i * 16, 16), 16)
        v = tok[strip, :].astype(F32)
        ms = jnp.mean(v * v, axis=-1, keepdims=True)
        normed[strip, :] = (v * lax.rsqrt(ms + EPS) * ngain).astype(BF16)

    pl.semaphore_wait(barrier, 2 * (SIDE - 1) + NTP - 1)
    for p in range(2):
        own_right(p).start()
        own_left(p).start()
    for p in range(2):
        cross(p, 0).start()

    ogbuf[tp] = ogain_ref[...]

    def og_copy(k, frm, to):
        return remote(ogain_ref, ogbuf.at[frm], og_s.at[k], og_r.at[k], ep, to)

    @pl.loop(1, NTP)
    def _(k):
        og_copy(k, tp, (tp + k) % NTP).start()

    class Exchange:
        def __init__(self, src, via, dst, sems, sign):
            self.src, self.via, self.dst, self.sems, self.sign = src, via, dst, sems, sign

        def to(self, a, b):
            return offset(a, b) if self.sign > 0 else offset((SIDE - a) % SIDE, (SIDE - b) % SIDE)

        def first(self, a, stays):
            part = pl.ds(a * rows_g, cap) if stays else pl.ds(a * rows_g + cap, rows_g - cap)
            dst = self.dst.at[part, :] if stays else self.via.at[a - 1]
            s_sem, r_sem = self.sems[0].at[a, stays], self.sems[1].at[a, stays]
            return remote(self.src.at[part, :], dst, s_sem, r_sem, self.to(a, 0), tp)

        def second(self, a, b):
            part = pl.ds(a * rows_g + b * cap, cap)
            src = self.via.at[a - 1, pl.ds((b - 1) * cap, cap), :] if a else self.src.at[part, :]
            return remote(src, self.dst.at[part, :], self.sems[2].at[a, b], self.sems[3].at[a, b], self.to(0, b), tp)

        def send(self, a):
            if a:
                for stays in range(2):
                    self.first(a, stays).start()
            else:
                for b in (2, 1, 3):
                    self.second(0, b).start()

        def forward(self, a):
            self.first(a, 0).wait_recv()
            for b in (2, 1, 3):
                self.second(a, b).start()

        def here(self, a):
            if a:
                self.first(a, 1).wait_recv()
            for b in (1, 3, 2):
                self.second(a, b).wait_recv()

        def drain(self):
            for a in range(SIDE):
                if a:
                    for stays in range(2):
                        self.first(a, stays).wait_send()
                for b in range(1, SIDE):
                    self.second(a, b).wait_send()

    out = Exchange(snd, mid, xbuf, (a_s, a_r, b_s, b_r), 1)
    back = Exchange(res, mid_back, ret, (c_s, c_r, d_s, d_r), -1)

    for a in SENT:
        group = pl.ds(a * rows_g, rows_g)

        @pl.loop(0, tiles)
        def _(n):
            cols = pl.ds(pl.multiple_of(n * 256, 256), 256)
            picked = dot(pbuf[group, :], normed[:, cols]).astype(BF16)
            snd[group, cols] = picked
            if a == 0:
                xbuf[0:cap, cols] = picked[0:cap, :]

        out.send(a)

    @pl.loop(0, NEP // 2)
    def _(q):
        halves = [
            jnp.where(
                vref[pl.ds(2 * q + h, 1), :] == slot_iota, gref[pl.ds(2 * q + h, 1), :], 0.0
            )
            for h in range(2)
        ]
        w = jnp.concatenate(halves, axis=0).T
        cols = pl.ds(pl.multiple_of(q * 2 * cap, 2 * cap), 2 * cap)
        for s in range(3):
            term = w.astype(BF16)
            wmat[s * toks : (s + 1) * toks, cols] = term
            w = w - term.astype(F32)

    def gate_up(g, j):
        rows = pl.ds(pl.multiple_of(g * rows_g, rows_g), rows_g)
        xg = xbuf[rows, :]
        gate_part = dot(xg, jnp.concatenate([wg[2 * j], wg[2 * j + 1]], axis=1))
        up_part = dot(xg, jnp.concatenate([wu[2 * j], wu[2 * j + 1]], axis=1))
        gl = jnp.minimum(gate_part, LIMIT)
        li = jnp.clip(up_part, -LIMIT, LIMIT)
        fresh = gl * jax.nn.sigmoid(ALPHA * gl) * (li + 1.0)
        act[rows, pl.ds(pl.multiple_of(j * 2 * unit, 2 * unit), 2 * unit)] = fresh.astype(BF16)

    def pass_on(p, first):
        own_right(p).wait_recv()
        own_left(p).wait_recv()
        relay(p).start()
        cross(p, 1).start()
        cross(p, 2).start()
        if first:
            own_right(2).start()
            own_left(2).start()
            cross(2, 0).start()

    pass_on(0, True)
    out.forward(1)
    out.forward(3)
    load_w[0].wait()
    load_w[1].wait()
    from_partner(0, 0).wait_recv()
    from_partner(1, 0).wait_recv()
    out.here(0)
    gate_up(0, 0)
    pass_on(1, False)
    out.forward(2)
    for p in range(2):
        for j in (1, 2):
            from_partner(p, j).wait_recv()

    @pl.loop(1, 3)
    def _(j):
        gate_up(0, j)

    out.here(1)

    @pl.loop(0, 3)
    def _(j):
        gate_up(1, j)

    relay(0).wait_recv()
    cross(0, 3).start()
    pass_on(2, False)
    out.here(3)

    @pl.loop(0, 3)
    def _(j):
        gate_up(3, j)

    def down(a):
        rows = pl.ds(a * rows_g, rows_g)

        @pl.loop(0, tiles)
        def _(n):
            cols = pl.ds(pl.multiple_of(n * 256, 256), 256)
            w_tile = wd[:, :, cols].reshape(NTP * unit, 256)
            done = dot(act[rows, :], w_tile).astype(BF16)
            res[rows, cols] = done
            if a == 0:
                ret[0:cap, cols] = done[0:cap, :]

        back.send(a)

    relay(1).wait_recv()
    cross(1, 3).start()
    for p in range(2):
        from_partner(p, 3).wait_recv()
    gate_up(0, 3)
    gate_up(1, 3)
    gate_up(3, 3)
    relay(2).wait_recv()
    cross(2, 3).start()
    load_w[2].wait()
    for j in range(SIDE - 1):
        from_partner(2, j).wait_recv()
    from_partner(2, 3).wait_recv()
    down(0)
    down(1)
    down(3)
    out.here(2)

    @pl.loop(0, SIDE)
    def _(j):
        gate_up(2, j)

    down(2)

    for a in SENT[:-1]:
        back.forward(a)

    for g in (0, 1, 3, 2):
        back.here(g)
        rows = pl.ds(g * rows_g, rows_g)

        @pl.loop(0, tiles)
        def _(n):
            cols = pl.ds(pl.multiple_of(n * 256, 256), 256)
            terms = dot(wmat[:, rows], ret[rows, cols])
            total = terms[0:toks] + terms[toks : 2 * toks] + terms[2 * toks : 3 * toks]
            if g == 0:
                comb[:, cols] = total
            else:
                comb[:, cols] += total

    @pl.loop(1, NTP)
    def _(k):
        og_copy(k, (tp + NTP - k) % NTP, (tp + k) % NTP).wait()

    @pl.loop(0, toks // 16)
    def _(i):
        strip = pl.ds(pl.multiple_of(i * 16, 16), 16)
        v = comb[strip, :]
        scale = lax.rsqrt(jnp.mean(v * v, axis=-1, keepdims=True) + EPS)
        for t in range(NTP):
            part = v[:, t * slice_w : (t + 1) * slice_w]
            mix[t, strip, :] = (part * scale * ogbuf[t]).astype(BF16)

    def fin(k, frm, to):
        at = pl.ds(pl.multiple_of(frm * toks, toks), toks)
        return remote(mix.at[to], out_hbm.at[at, :], fin_s.at[k], fin_r.at[k], ep, to)

    @pl.loop(1, NTP)
    def _(k):
        fin(k, tp, (tp + k) % NTP).start()

    keep = pltpu.make_async_copy(mix.at[tp], out_hbm.at[own, :], loc_sem.at[4])
    keep.start()

    for p in range(3):
        own_right(p).wait_send()
        own_left(p).wait_send()
        relay(p).wait_send()
        for j in range(SIDE):
            cross(p, j).wait_send()

    out.drain()
    back.drain()

    @pl.loop(1, NTP)
    def _(k):
        fin(k, (tp + NTP - k) % NTP, (tp + k) % NTP).wait()

    keep.wait()


def local(tokens, expert_ids, gate_values, norm_gain, gate_weight, up_weight, down_weight, out_gain):
    toks, width = tokens.shape
    cap = toks // 2
    slots = NEP * cap
    unit = gate_weight.shape[2]
    hidden = NTP * unit
    slice_w = width // NTP
    vmem, hbm = pltpu.VMEM, pl.BlockSpec(memory_space=pl.ANY)
    in_vmem = pl.BlockSpec(memory_space=pltpu.VMEM)
    dma = pltpu.SemaphoreType.DMA
    return pl.pallas_call(
        kernel,
        out_shape=jax.ShapeDtypeStruct((NTP * toks, slice_w), BF16),
        in_specs=[hbm, in_vmem, in_vmem, in_vmem, hbm, hbm, hbm, in_vmem],
        out_specs=hbm,
        scratch_shapes=[
            vmem((toks, width), BF16),
            vmem((toks, width), BF16),
            vmem((slots, toks), BF16),
            vmem((NEP, toks), F32),
            vmem((NEP, toks), F32),
            vmem((slots, width), BF16),
            vmem((slots, width), BF16),
            vmem((SIDE - 1, 3 * cap, width), BF16),
            vmem((NTP, width, unit), BF16),
            vmem((NTP, width, unit), BF16),
            vmem((NTP, unit, width), BF16),
            vmem((slots, hidden), BF16),
            vmem((slots, width), BF16),
            vmem((slots, width), BF16),
            vmem((SIDE - 1, 3 * cap, width), BF16),
            vmem((3 * toks, slots), BF16),
            vmem((toks, width), F32),
            vmem((NTP, toks, slice_w), BF16),
            vmem((NTP, 1, slice_w), F32),
            dma((5,)), dma((3,)), dma((3,)), dma((3,)), dma((3, SIDE)), dma((3, 3)), dma((3, SIDE)),
            dma((SIDE, 2)), dma((SIDE, 2)), dma((SIDE, SIDE)), dma((SIDE, SIDE)),
            dma((SIDE, 2)), dma((SIDE, 2)), dma((SIDE, SIDE)), dma((SIDE, SIDE)),
            dma((NTP,)), dma((NTP,)), dma((NTP,)), dma((NTP,)),
        ],
        compiler_params=pltpu.CompilerParams(
            collective_id=0, has_side_effects=True, vmem_limit_bytes=60000 * 1024
        ),
    )(
        tokens, expert_ids.T, gate_values.T, norm_gain.reshape(1, width),
        gate_weight, up_weight, down_weight, out_gain.reshape(1, slice_w),
    )


def solution(mesh):
    in_specs = (
        P(("ep", "tp"), None), P("ep", None), P("ep", None), P(),
        P("ep", None, "tp"), P("ep", None, "tp"), P("ep", "tp", None), P("tp"),
    )
    return jax.shard_map(
        local, mesh=mesh, in_specs=in_specs, out_specs=P("ep", "tp"), check_vma=False
    )
```

```python
import jax
import jax.numpy as jnp
from jax import lax
from jax.experimental import pallas as pl
from jax.experimental.pallas import tpu as pltpu
from jax.sharding import PartitionSpec as P

MESH = pl.DeviceIdType.MESH
F32, BF16 = jnp.float32, jnp.bfloat16
EPS = 1e-05
LIMIT = 7.0
ALPHA = 1.702
SIDE = 4
NEP, NTP = 16, 8
SENT = (1, 3, 2, 0)


def dot(a, b):
    return jnp.dot(a, b, preferred_element_type=F32)


def kernel(
    tok_hbm, ids_ref, gates_ref, ngain_ref, wg_hbm, wu_hbm, wd_hbm, ogain_ref, out_hbm,
    tok, normed, pbuf, vref, gref, snd, xbuf, mid, wg, wu, wd, act, res, ret, mid_back, wmat, comb, mix, ogbuf,
    loc_sem, wl_s, wr_s, wy_s, wc_s, wi_r, wc_r, a_s, a_r, b_s, b_r, c_s, c_r, d_s, d_r, fin_s, fin_r, og_s, og_r,
):
    toks, width = tok.shape
    cap = toks // 2
    rows_g = SIDE * cap
    unit = wg.shape[2]
    slice_w = mix.shape[2]
    tiles = width // 256

    ep = lax.axis_index("ep")
    tp = lax.axis_index("tp")
    z, x = ep // SIDE, ep % SIDE
    y, core = tp // 2, tp % 2

    def peer(dz, dx):
        return ((z + dz) % SIDE) * SIDE + (x + dx) % SIDE

    def offset(a, b):
        return peer(core * a + (1 - core) * b, (1 - core) * a + core * b)

    right = ((y + 1) % SIDE) * 2 + core
    left = ((y + SIDE - 1) % SIDE) * 2 + core
    partner = y * 2 + 1 - core

    barrier = pltpu.get_barrier_semaphore()

    @pl.loop(1, SIDE)
    def _(r):
        for to in (peer(r, 0), peer(0, r)):
            pl.semaphore_signal(barrier, inc=1, device_id=(to, tp), device_id_type=MESH)

    @pl.loop(1, NTP)
    def _(k):
        pl.semaphore_signal(barrier, inc=1, device_id=(ep, (tp + k) % NTP), device_id_type=MESH)

    load_tok = pltpu.make_async_copy(tok_hbm, tok, loc_sem.at[0])
    load_tok.start()
    bufs = (wg, wu, wd)
    srcs = (wg_hbm.at[0], wu_hbm.at[0], wd_hbm.at[0])
    load_w = [
        pltpu.make_async_copy(srcs[p], bufs[p].at[core], loc_sem.at[1 + p]) for p in range(3)
    ]
    for cp in load_w:
        cp.start()

    def remote(src, dst, send, recv, ep_to, tp_to):
        return pltpu.make_async_remote_copy(
            src_ref=src, dst_ref=dst, send_sem=send, recv_sem=recv,
            device_id=(ep_to, tp_to), device_id_type=MESH,
        )

    def own_right(p):
        return remote(srcs[p], bufs[p].at[2 + core], wr_s.at[p], wi_r.at[p, 0], ep, right)

    def own_left(p):
        return remote(srcs[p], bufs[p].at[4 + core], wl_s.at[p], wi_r.at[p, 1], ep, left)

    def relay(p):
        return remote(
            bufs[p].at[2 + 2 * core + core], bufs[p].at[6 + core], wy_s.at[p], wi_r.at[p, 2],
            ep, right + core * (left - right),
        )

    def cross(p, j):
        src = srcs[p] if j == 0 else bufs[p].at[2 * j + core]
        return remote(src, bufs[p].at[2 * j + core], wc_s.at[p, j], wc_r.at[p, j], ep, partner)

    def from_partner(p, j):
        slot = bufs[p].at[2 * j + 1 - core]
        return remote(slot, slot, wc_s.at[p, j], wc_r.at[p, j], ep, partner)

    own = pl.ds(pl.multiple_of(tp * toks, toks), toks)
    ids = ids_ref[:, own]
    gates = gates_ref[:, own]
    place = lax.broadcasted_iota(jnp.int32, (NEP, toks), 0)
    expert = jnp.zeros((NEP, toks), jnp.int32)
    for p in range(NEP):
        expert = jnp.where(place == p, offset(p // SIDE, p % SIDE), expert)
    named = jnp.zeros((NEP, toks), F32)
    gate_of = jnp.zeros((NEP, toks), F32)
    for k in range(ids.shape[0]):
        hit = ids[k : k + 1, :] == expert
        named = jnp.where(hit, 1.0, named)
        gate_of = jnp.where(hit, gates[k : k + 1, :], gate_of)
    t_from = lax.broadcasted_iota(jnp.int32, (toks, toks), 0)
    t_to = lax.broadcasted_iota(jnp.int32, (toks, toks), 1)
    earlier = jnp.where(t_from < t_to, 1.0, 0.0).astype(BF16)
    slot = dot(named.astype(BF16), earlier)
    vref[...] = jnp.where(named > 0.0, slot, -1.0)
    gref[...] = gate_of
    slot_iota = lax.broadcasted_iota(jnp.int32, (cap, toks), 0).astype(F32)

    @pl.loop(0, NEP)
    def _(r):
        pick = jnp.where(vref[pl.ds(r, 1), :] == slot_iota, 1.0, 0.0)
        pbuf[pl.ds(pl.multiple_of(r * cap, cap), cap), :] = pick.astype(BF16)

    load_tok.wait()
    ngain = ngain_ref[...]

    @pl.loop(0, toks // 16)
    def _(i):
        strip = pl.ds(pl.multiple_of(i * 16, 16), 16)
        v = tok[strip, :].astype(F32)
        ms = jnp.mean(v * v, axis=-1, keepdims=True)
        normed[strip, :] = (v * lax.rsqrt(ms + EPS) * ngain).astype(BF16)

    pl.semaphore_wait(barrier, 2 * (SIDE - 1) + NTP - 1)
    def relay_half(h):
        part = pl.ds(h * (unit // 2), unit // 2)
        return remote(
            wd.at[2 + 3 * core, part, :], wd.at[6 + core, part, :], wy_s.at[2 + h], wi_r.at[2, 2 + h],
            ep, right + core * (left - right),
        )

    def cross_half(h, lane):
        part = wd.at[6 + lane, pl.ds(h * (unit // 2), unit // 2), :]
        return remote(part, part, wc_s.at[2, 3 + h], wc_r.at[2, 3 + h], ep, partner)

    for p in range(2):
        own_right(p).start()
        own_left(p).start()
    for p in range(2):
        cross(p, 0).start()

    ogbuf[tp] = ogain_ref[...]

    def og_copy(k, frm, to):
        return remote(ogain_ref, ogbuf.at[frm], og_s.at[k], og_r.at[k], ep, to)

    @pl.loop(1, NTP)
    def _(k):
        og_copy(k, tp, (tp + k) % NTP).start()

    class Exchange:
        def __init__(self, src, via, dst, sems, sign):
            self.src, self.via, self.dst, self.sems, self.sign = src, via, dst, sems, sign

        def to(self, a, b):
            return offset(a, b) if self.sign > 0 else offset((SIDE - a) % SIDE, (SIDE - b) % SIDE)

        def first(self, a, stays):
            part = pl.ds(a * rows_g, cap) if stays else pl.ds(a * rows_g + cap, rows_g - cap)
            dst = self.dst.at[part, :] if stays else self.via.at[a - 1]
            s_sem, r_sem = self.sems[0].at[a, stays], self.sems[1].at[a, stays]
            return remote(self.src.at[part, :], dst, s_sem, r_sem, self.to(a, 0), tp)

        def second(self, a, b):
            part = pl.ds(a * rows_g + b * cap, cap)
            src = self.via.at[a - 1, pl.ds((b - 1) * cap, cap), :] if a else self.src.at[part, :]
            return remote(src, self.dst.at[part, :], self.sems[2].at[a, b], self.sems[3].at[a, b], self.to(0, b), tp)

        def send(self, a):
            if a:
                for stays in range(2):
                    self.first(a, stays).start()
            else:
                for b in (2, 1, 3):
                    self.second(0, b).start()

        def forward(self, a):
            self.first(a, 0).wait_recv()
            for b in (2, 1, 3):
                self.second(a, b).start()

        def here(self, a):
            if a:
                self.first(a, 1).wait_recv()
            for b in (1, 3, 2):
                self.second(a, b).wait_recv()

        def drain(self):
            for a in range(SIDE):
                if a:
                    for stays in range(2):
                        self.first(a, stays).wait_send()
                for b in range(1, SIDE):
                    self.second(a, b).wait_send()

    out = Exchange(snd, mid, xbuf, (a_s, a_r, b_s, b_r), 1)
    back = Exchange(res, mid_back, ret, (c_s, c_r, d_s, d_r), -1)

    for a in SENT:
        group = pl.ds(a * rows_g, rows_g)

        @pl.loop(0, tiles)
        def _(n):
            cols = pl.ds(pl.multiple_of(n * 256, 256), 256)
            picked = dot(pbuf[group, :], normed[:, cols]).astype(BF16)
            snd[group, cols] = picked
            if a == 0:
                xbuf[0:cap, cols] = picked[0:cap, :]

        out.send(a)

    @pl.loop(0, NEP // 2)
    def _(q):
        halves = [
            jnp.where(
                vref[pl.ds(2 * q + h, 1), :] == slot_iota, gref[pl.ds(2 * q + h, 1), :], 0.0
            )
            for h in range(2)
        ]
        w = jnp.concatenate(halves, axis=0).T
        cols = pl.ds(pl.multiple_of(q * 2 * cap, 2 * cap), 2 * cap)
        for s in range(3):
            term = w.astype(BF16)
            wmat[s * toks : (s + 1) * toks, cols] = term
            w = w - term.astype(F32)

    def gate_up(g, j):
        rows = pl.ds(pl.multiple_of(g * rows_g, rows_g), rows_g)
        xg = xbuf[rows, :]
        gate_part = dot(xg, jnp.concatenate([wg[2 * j], wg[2 * j + 1]], axis=1))
        up_part = dot(xg, jnp.concatenate([wu[2 * j], wu[2 * j + 1]], axis=1))
        gl = jnp.minimum(gate_part, LIMIT)
        li = jnp.clip(up_part, -LIMIT, LIMIT)
        fresh = gl * jax.nn.sigmoid(ALPHA * gl) * (li + 1.0)
        act[rows, pl.ds(pl.multiple_of(j * 2 * unit, 2 * unit), 2 * unit)] = fresh.astype(BF16)

    def pass_on(p, first):
        own_right(p).wait_recv()
        own_left(p).wait_recv()
        if p < 2:
            relay(p).start()
        else:
            for h in range(2):
                relay_half(h).start()
        cross(p, 1).start()
        cross(p, 2).start()
        if first:
            own_right(2).start()
            own_left(2).start()
            cross(2, 0).start()

    pass_on(0, True)
    out.forward(1)
    out.forward(3)
    load_w[0].wait()
    load_w[1].wait()
    from_partner(0, 0).wait_recv()
    from_partner(1, 0).wait_recv()
    out.here(0)
    gate_up(0, 0)
    pass_on(1, False)
    out.forward(2)
    for p in range(2):
        for j in (1, 2):
            from_partner(p, j).wait_recv()

    @pl.loop(1, 3)
    def _(j):
        gate_up(0, j)

    out.here(1)

    @pl.loop(0, 3)
    def _(j):
        gate_up(1, j)

    relay(0).wait_recv()
    cross(0, 3).start()
    pass_on(2, False)
    out.here(3)

    @pl.loop(0, 3)
    def _(j):
        gate_up(3, j)

    def down(a):
        rows = pl.ds(a * rows_g, rows_g)

        @pl.loop(0, tiles // 2)
        def _(n):
            cols = pl.ds(pl.multiple_of(n * 512, 512), 512)
            w_tile = wd[:, :, cols].reshape(NTP * unit, 512)
            done = dot(act[rows, :], w_tile).astype(BF16)
            res[rows, cols] = done
            if a == 0:
                ret[0:cap, cols] = done[0:cap, :]

        back.send(a)

    relay(1).wait_recv()
    cross(1, 3).start()
    for p in range(2):
        from_partner(p, 3).wait_recv()
    gate_up(0, 3)
    gate_up(1, 3)
    gate_up(3, 3)
    for h in range(2):
        relay_half(h).wait_recv()
        cross_half(h, core).start()
    load_w[2].wait()
    for j in range(SIDE - 1):
        from_partner(2, j).wait_recv()
    for h in range(2):
        cross_half(h, 1 - core).wait_recv()
    down(0)
    down(1)
    down(3)
    out.here(2)

    @pl.loop(0, SIDE)
    def _(j):
        gate_up(2, j)

    down(2)

    for a in SENT[:-1]:
        back.forward(a)

    for g in (0, 1, 3, 2):
        back.here(g)
        rows = pl.ds(g * rows_g, rows_g)

        @pl.loop(0, tiles)
        def _(n):
            cols = pl.ds(pl.multiple_of(n * 256, 256), 256)
            terms = dot(wmat[:, rows], ret[rows, cols])
            total = terms[0:toks] + terms[toks : 2 * toks] + terms[2 * toks : 3 * toks]
            if g == 0:
                comb[:, cols] = total
            else:
                comb[:, cols] += total

    @pl.loop(1, NTP)
    def _(k):
        og_copy(k, (tp + NTP - k) % NTP, (tp + k) % NTP).wait()

    half = toks // 2

    def fin(k, h, frm, to):
        at = pl.ds(pl.multiple_of(frm * toks + h * half, half), half)
        src = mix.at[to, pl.ds(h * half, half), :]
        return remote(src, out_hbm.at[at, :], fin_s.at[k, h], fin_r.at[k, h], ep, to)

    for h in range(2):

        @pl.loop(h * half // 16, (h + 1) * half // 16)
        def _(i):
            strip = pl.ds(pl.multiple_of(i * 16, 16), 16)
            v = comb[strip, :]
            scale = lax.rsqrt(jnp.mean(v * v, axis=-1, keepdims=True) + EPS)
            for t in range(NTP):
                part = v[:, t * slice_w : (t + 1) * slice_w]
                mix[t, strip, :] = (part * scale * ogbuf[t]).astype(BF16)

        @pl.loop(1, NTP)
        def _(k):
            fin(k, h, tp, (tp + k) % NTP).start()

    keep = pltpu.make_async_copy(mix.at[tp], out_hbm.at[own, :], loc_sem.at[4])
    keep.start()

    for p in range(3):
        own_right(p).wait_send()
        own_left(p).wait_send()
        if p < 2:
            relay(p).wait_send()
        for j in range(SIDE if p < 2 else SIDE - 1):
            cross(p, j).wait_send()
    for h in range(2):
        relay_half(h).wait_send()
        cross_half(h, core).wait_send()

    out.drain()
    back.drain()

    @pl.loop(1, NTP)
    def _(k):
        for h in range(2):
            fin(k, h, (tp + NTP - k) % NTP, (tp + k) % NTP).wait()

    keep.wait()


def local(tokens, expert_ids, gate_values, norm_gain, gate_weight, up_weight, down_weight, out_gain):
    toks, width = tokens.shape
    cap = toks // 2
    slots = NEP * cap
    unit = gate_weight.shape[2]
    hidden = NTP * unit
    slice_w = width // NTP
    vmem, hbm = pltpu.VMEM, pl.BlockSpec(memory_space=pl.ANY)
    in_vmem = pl.BlockSpec(memory_space=pltpu.VMEM)
    dma = pltpu.SemaphoreType.DMA
    return pl.pallas_call(
        kernel,
        out_shape=jax.ShapeDtypeStruct((NTP * toks, slice_w), BF16),
        in_specs=[hbm, in_vmem, in_vmem, in_vmem, hbm, hbm, hbm, in_vmem],
        out_specs=hbm,
        scratch_shapes=[
            vmem((toks, width), BF16),
            vmem((toks, width), BF16),
            vmem((slots, toks), BF16),
            vmem((NEP, toks), F32),
            vmem((NEP, toks), F32),
            vmem((slots, width), BF16),
            vmem((slots, width), BF16),
            vmem((SIDE - 1, 3 * cap, width), BF16),
            vmem((NTP, width, unit), BF16),
            vmem((NTP, width, unit), BF16),
            vmem((NTP, unit, width), BF16),
            vmem((slots, hidden), BF16),
            vmem((slots, width), BF16),
            vmem((slots, width), BF16),
            vmem((SIDE - 1, 3 * cap, width), BF16),
            vmem((3 * toks, slots), BF16),
            vmem((toks, width), F32),
            vmem((NTP, toks, slice_w), BF16),
            vmem((NTP, 1, slice_w), F32),
            dma((5,)), dma((3,)), dma((3,)), dma((4,)), dma((3, SIDE + 1)), dma((3, 4)), dma((3, SIDE + 1)),
            dma((SIDE, 2)), dma((SIDE, 2)), dma((SIDE, SIDE)), dma((SIDE, SIDE)),
            dma((SIDE, 2)), dma((SIDE, 2)), dma((SIDE, SIDE)), dma((SIDE, SIDE)),
            dma((NTP, 2)), dma((NTP, 2)), dma((NTP,)), dma((NTP,)),
        ],
        compiler_params=pltpu.CompilerParams(
            collective_id=0, has_side_effects=True, vmem_limit_bytes=60000 * 1024
        ),
    )(
        tokens, expert_ids.T, gate_values.T, norm_gain.reshape(1, width),
        gate_weight, up_weight, down_weight, out_gain.reshape(1, slice_w),
    )


def solution(mesh):
    in_specs = (
        P(("ep", "tp"), None), P("ep", None), P("ep", None), P(),
        P("ep", None, "tp"), P("ep", None, "tp"), P("ep", "tp", None), P("tp"),
    )
    return jax.shard_map(
        local, mesh=mesh, in_specs=in_specs, out_specs=P("ep", "tp"), check_vma=False
    )
```
